512 devices in a mesh: grp: 2 (over y), sp: 32 (over z), tp: 8 (over x, core).
Axes of the slice: x: 4, y: 2, z: 32, core: 2. Of those that a mesh axis runs over, the one named last changes fastest.
The devices are a block of a 4x8x32 slice.
Arguments:
- stream: bfloat16 [49152, 4096], P(('grp', 'sp'), 'tp'), parts along dimension 0, may hold values from -400 to 400
- in_weight: bfloat16 [2, 1024, 4096], P(None, 'sp', 'tp'), may hold values from -0.09375 to 0.09375
- out_weight: bfloat16 [2, 1024, 4096], P(None, 'sp', 'tp'), may hold values from -0.1875 to 0.1875
- group_mix: bfloat16 [2, 4, 256, 256], replicated, may hold values from -0.375 to 0.375
- pool_gain: float32 [2, 1024], replicated, may hold values from 0.1 to 1.9
- norm_gain: float32 [2, 4096], P(None, 'tp'), may hold values from 0.1 to 1.9
- norm_shift: float32 [2, 4096], P(None, 'tp'), may hold values from -3 to 3
Outputs:
- refined: bfloat16 [49152, 4096], P(('grp', 'sp'), 'tp'), parts along dimension 0
The draws below stay inside these ranges and needn't reach their ends.
There are 2 independent parts, one for each index of `grp`. The reference program is written for one: setup_inputs(seed, part) draws one part's arguments, and reference() takes and returns one part's arrays. A program takes and returns all parts, laid end to end along the dimension named above; an argument that names none is the same for every part. Nothing has to cross between parts.
All inputs are finite; a program needn't handle non-finite values.
Results may differ from the reference program's by a relative error of at most 0.015.
Values may be sent and summed in bfloat16 or wider, within the bound.
No kernel may reach another device: no remote copies, remote signals or barrier semaphores. Data moves between devices by JAX's collectives and lax.ppermute only.
A program may use at most 64 MiB of HBM per device.

```python
import jax
import jax.numpy as jnp
from jax import lax

D = 4096
POOL = 1024
GROUPS = 4
GROUP_WIDTH = 256
LAYERS = 2
TOKENS = 24576
N_TP = 8


def draw_stream(key, part):
    base = jax.random.fold_in(key, 17)
    first_key, second_key = jax.random.split(base, 2)
    column = jnp.arange(D, dtype=jnp.float32) / D
    row_scale = 10.0 ** jax.random.uniform(second_key, (TOKENS, 1), jnp.float32)
    entries = jnp.clip(jax.random.normal(first_key, (TOKENS, D), jnp.float32), -4.0, 4.0)
    column_scale = 10.0 ** column
    return (entries * column_scale[None, :] * row_scale).astype(jnp.bfloat16)


def steps_of(rng, extent, cuts, smallest, high):
    factor_of, own = 1.0, jax.random.fold_in(rng, 6)
    for axis_at, shards_of in cuts:
        steps = jnp.exp(jax.random.uniform(jax.random.fold_in(own, axis_at), (shards_of,), jnp.float32, smallest / len(cuts), high / len(cuts)))
        factor_of = factor_of * jnp.repeat(steps, extent[axis_at] // shards_of).reshape([-1 if axis == axis_at else 1 for axis in range(len(extent))])
    return factor_of


def centred(stream_key, dims, scale, bound, cuts=(), kind=jnp.bfloat16):
    array = jax.random.normal(stream_key, dims, jnp.float32) * scale
    if len(cuts) > 0:
        array = steps_of(stream_key, dims, cuts, -0.22, 0.18) * array
    return jnp.clip(array, min=-bound, max=bound).astype(kind)


def setup_inputs(seed: int = 0, part: int = 0) -> dict:
    seeds = jax.random.split(jax.random.key(seed), 8)
    own_keys = jax.random.split(jax.random.fold_in(seeds[7], part), 8)
    return {
        "stream": draw_stream(jax.random.fold_in(jax.random.fold_in(seeds[7], part), 71), part),
        "in_weight": centred(seeds[1], (LAYERS, POOL, D), D ** -0.5, 0.09375, ((1, 32), (2, 8))),
        "out_weight": centred(seeds[2], (LAYERS, POOL, D), POOL ** -0.5, 0.1875, ((1, 32), (2, 8))),
        "group_mix": centred(seeds[3], (LAYERS, GROUPS, GROUP_WIDTH, GROUP_WIDTH), GROUP_WIDTH ** -0.5, 0.375),
        "pool_gain": jnp.clip(1.0 + 0.18 * jax.random.normal(seeds[4], (LAYERS, POOL), jnp.float32), 0.1, 1.9),
        "norm_gain": jnp.clip(1.0 + 0.18 * jax.random.normal(seeds[5], (LAYERS, D), jnp.float32), 0.1, 1.9),
        "norm_shift": centred(seeds[6], (LAYERS, D), 0.5, 3.0, ((1, 8),), jnp.float32),
    }


epsilon = 1e-05

def reference(stream, in_weight, out_weight, group_mix, pool_gain, norm_gain, norm_shift):
    tokens_total = stream.shape[0]
    channel_block = D // N_TP
    alpha = (2.0 * LAYERS) ** 0.25
    current = stream
    for layer_index in range(LAYERS):
        hidden_sum = jnp.zeros((tokens_total, POOL), jnp.float32)
        for part_index in range(N_TP):
            lower = part_index * channel_block
            upper = lower + channel_block
            term = jnp.dot(current[:, lower:upper], in_weight[layer_index][:, lower:upper].T, preferred_element_type=jnp.float32)
            rounded = lax.optimization_barrier(term.astype(jnp.bfloat16))
            hidden_sum = hidden_sum + rounded.astype(jnp.float32)
        hidden = hidden_sum.astype(jnp.bfloat16)
        positions = jnp.arange(1, tokens_total + 1, dtype=jnp.float32)[:, None]
        pooled_pieces = []
        for group_index in range(GROUPS):
            width = 2 ** (group_index + 1)
            group_cols = hidden[:, group_index * GROUP_WIDTH:(group_index + 1) * GROUP_WIDTH].astype(jnp.float32)
            padded = jnp.pad(group_cols, ((width - 1, 0), (0, 0)))
            window_sum = jnp.zeros_like(group_cols)
            for offset in range(width):
                window_sum = window_sum + padded[offset:offset + tokens_total]
            counts = jnp.minimum(positions, float(width))
            pooled_pieces.append(window_sum / counts - group_cols)
        pooled = jnp.concatenate(pooled_pieces, axis=1).astype(jnp.bfloat16)
        mixed_pieces = []
        for group_index in range(GROUPS):
            group_rows = pooled[:, group_index * GROUP_WIDTH:(group_index + 1) * GROUP_WIDTH]
            mixed_pieces.append(jnp.dot(group_rows, group_mix[layer_index, group_index], preferred_element_type=jnp.float32))
        scaled = (jnp.concatenate(mixed_pieces, axis=1) * pool_gain[layer_index][None, :]).astype(jnp.bfloat16)
        branch = jnp.dot(scaled, out_weight[layer_index], preferred_element_type=jnp.float32)
        summed = alpha * current.astype(jnp.float32) + branch
        row_mean = lax.optimization_barrier(jnp.sum(summed, axis=1)) / D
        row_var = lax.optimization_barrier(jnp.sum(summed * summed, axis=1)) / D - row_mean * row_mean
        normed = (summed - row_mean[:, None]) * lax.rsqrt(row_var + epsilon)[:, None]
        current = (normed * norm_gain[layer_index][None, :] + norm_shift[layer_index][None, :]).astype(jnp.bfloat16)
    return current
```

```python
import jax
import jax.numpy as jnp
from jax import lax
from jax.sharding import PartitionSpec as P

D = 4096
POOL = 1024
GROUPS = 4
GROUP_WIDTH = 256
LAYERS = 2
HALO = 32

epsilon = 1e-05


def shifted(x, axis, distance):
    n = lax.axis_size(axis)
    return lax.ppermute(x, axis, [(i, (i + distance) % n) for i in range(n)])


def swapped(x, axis):
    n = lax.axis_size(axis)
    return lax.ppermute(x, axis, [(i, i ^ 1) for i in range(n)])


def chips():
    n = lax.axis_size("tp")
    return [[core + 2 * i for i in range(n // 2)] for core in range(2)]


def every_other():
    n = lax.axis_size("sp")
    return [[first + 2 * i for i in range(n // 2)] for first in range(2)]


def between_chips(x):
    return lax.all_to_all(
        x, "tp", split_axis=0, concat_axis=0, axis_index_groups=chips(), tiled=True
    )


def ordered(first, second, flip, axis):
    return jnp.where(
        flip,
        jnp.concatenate([second, first], axis=axis),
        jnp.concatenate([first, second], axis=axis),
    )


def halves_swapped(x, flip):
    half = x.shape[-1] // 2
    return ordered(x[..., :half], x[..., half:], flip, -1)


def all_channels(own_half):
    rows = own_half.shape[0]
    low = shifted(own_half[: rows // 2], "sp", 1)
    high = shifted(own_half[rows // 2 :], "sp", -1)
    other_half = jnp.concatenate([low, high], axis=0)
    partner_own = swapped(own_half, "tp")
    partner_other = swapped(other_half, "tp")
    return own_half, other_half, partner_own, partner_other


def delayed(x, rows):
    return jnp.pad(x[: x.shape[0] - rows], ((rows, 0), (0, 0)))


def pooled_windows(hidden, group, positions):
    values = jnp.where(positions >= 0, hidden, 0).astype(jnp.float32)
    running = values
    window_sums = jnp.zeros_like(values)
    for octave in range(GROUPS):
        running = running + delayed(running, 2**octave)
        window_sums = jnp.where(group == octave, running, window_sums)
    width = jnp.left_shift(2, group)
    counts = jnp.clip(positions + 1, 1, width).astype(jnp.float32)
    return (window_sums / counts - values).astype(jnp.bfloat16)


def per_device(stream, in_weight, out_weight, group_mix, pool_gain, norm_gain, norm_shift):
    tok_rows, width = stream.shape
    tok_half = tok_rows // 2
    at_sp = lax.axis_index("sp")
    at_tp = lax.axis_index("tp")
    core = at_tp % 2
    group = at_tp // 2
    odd = at_sp % 2
    flip = odd == 1
    alpha = (2.0 * LAYERS) ** 0.25

    weights = jnp.stack([in_weight[0], out_weight[0], in_weight[1], out_weight[1]])
    split = width // 2
    keep = jnp.where(flip, weights[..., split:], weights[..., :split])
    give = jnp.where(flip, weights[..., :split], weights[..., split:])
    traded = swapped(give, "sp")
    pair = ordered(keep, traded, flip, 1)
    first_in = lax.all_gather(
        pair[0], "sp", axis=0, axis_index_groups=every_other(), tiled=True
    )
    later = lax.all_gather(
        pair[1:], "sp", axis=1, axis_index_groups=every_other(), tiled=True
    )

    earlier = lax.ppermute(
        stream[tok_rows - HALO :],
        "sp",
        [(i, i + 1) for i in range(lax.axis_size("sp") - 1)],
    )
    extended = jnp.concatenate([earlier, stream], axis=0)
    rows = tok_half + HALO
    mine = lax.dynamic_slice_in_dim(extended, core * tok_half, rows, 0)
    theirs = lax.dynamic_slice_in_dim(extended, (1 - core) * tok_half, rows, 0)
    partners = swapped(theirs, "tp")
    current = jnp.concatenate(
        [halves_swapped(mine, flip), halves_swapped(partners, flip)], axis=1
    )
    norms = jnp.stack([norm_gain, norm_shift])
    norms = jnp.concatenate(
        [halves_swapped(norms, flip), halves_swapped(swapped(norms, "tp"), flip)], axis=-1
    )
    positions = (
        at_sp * tok_rows + core * tok_half - HALO + jnp.arange(rows, dtype=jnp.int32)
    )[:, None]

    chip_count = lax.axis_size("tp") // 2
    for layer_index in range(LAYERS):
        in_quarters = all_channels(first_in if layer_index == 0 else later[1])
        whole_in = jnp.concatenate(in_quarters, axis=1).reshape(GROUPS, GROUP_WIDTH, 2 * width)
        partial = jnp.einsum(
            "tc,goc->gto", current, whole_in, preferred_element_type=jnp.float32
        ).astype(jnp.bfloat16)
        hidden = (
            between_chips(partial).astype(jnp.float32).sum(axis=0).astype(jnp.bfloat16)
        )
        pooled = pooled_windows(hidden, group, positions)
        mixed = jnp.dot(
            pooled,
            lax.dynamic_index_in_dim(group_mix[layer_index], group, 0, keepdims=False),
            preferred_element_type=jnp.float32,
        )
        gains = lax.dynamic_slice_in_dim(
            pool_gain[layer_index], group * GROUP_WIDTH, GROUP_WIDTH
        )
        scaled = (mixed * gains[None, :]).astype(jnp.bfloat16)
        everyone = between_chips(
            jnp.broadcast_to(scaled, (chip_count, *scaled.shape))
        )
        out_quarters = all_channels(later[0 if layer_index == 0 else 2])
        whole_out = jnp.concatenate(out_quarters, axis=1).reshape(
            GROUPS, GROUP_WIDTH, 2 * width
        )
        branch = jnp.einsum(
            "gti,gic->tc", everyone, whole_out, preferred_element_type=jnp.float32
        )
        summed = alpha * current.astype(jnp.float32) + branch
        stats = jnp.stack([jnp.sum(summed, axis=1), jnp.sum(summed * summed, axis=1)])
        totals = between_chips(jnp.broadcast_to(stats, (chip_count, *stats.shape))).sum(axis=0)
        row_mean = totals[0] / D
        row_var = totals[1] / D - row_mean * row_mean
        normed = (summed - row_mean[:, None]) * lax.rsqrt(row_var + epsilon)[:, None]
        current = (
            normed * norms[0, layer_index][None, :] + norms[1, layer_index][None, :]
        ).astype(jnp.bfloat16)

    done = current[HALO:]
    own = halves_swapped(done[:, :width], flip)
    sent = halves_swapped(done[:, width:], flip)
    arrived = swapped(sent, "tp")
    return ordered(own, arrived, core == 1, 0)


def solution(mesh):
    in_specs = (
        P(("grp", "sp"), "tp"),
        P(None, "sp", "tp"),
        P(None, "sp", "tp"),
        P(),
        P(),
        P(None, "tp"),
        P(None, "tp"),
    )
    out_specs = P(("grp", "sp"), "tp")
    return jax.shard_map(
        per_device, mesh=mesh, in_specs=in_specs, out_specs=out_specs, check_vma=False
    )
```

```python
import jax
import jax.numpy as jnp
from jax import lax
from jax.sharding import PartitionSpec as P

D = 4096
POOL = 1024
GROUPS = 4
GROUP_WIDTH = 256
LAYERS = 2
HALO = 32

epsilon = 1e-05


def shifted(x, axis, distance):
    n = lax.axis_size(axis)
    return lax.ppermute(x, axis, [(i, (i + distance) % n) for i in range(n)])


def swapped(x, axis):
    n = lax.axis_size(axis)
    return lax.ppermute(x, axis, [(i, i ^ 1) for i in range(n)])


def chips():
    n = lax.axis_size("tp")
    return [[core + 2 * i for i in range(n // 2)] for core in range(2)]


def every_other():
    n = lax.axis_size("sp")
    return [[first + 2 * i for i in range(n // 2)] for first in range(2)]


def between_chips(x):
    return lax.all_to_all(
        x, "tp", split_axis=0, concat_axis=0, axis_index_groups=chips(), tiled=True
    )


def ordered(first, second, flip, axis):
    return jnp.where(
        flip,
        jnp.concatenate([second, first], axis=axis),
        jnp.concatenate([first, second], axis=axis),
    )


def halves_swapped(x, flip):
    half = x.shape[-1] // 2
    return ordered(x[..., :half], x[..., half:], flip, -1)


def all_channels(own_half):
    rows = own_half.shape[0]
    low = shifted(own_half[: rows // 2], "sp", 1)
    high = shifted(own_half[rows // 2 :], "sp", -1)
    partner_own = swapped(own_half, "tp")
    other_half = jnp.concatenate([low, high], axis=0)
    partner_other = swapped(other_half, "tp")
    return own_half, other_half, partner_own, partner_other


def after(x, earlier):
    return lax.optimization_barrier((x, earlier))[0]


def together(*arrays):
    return lax.optimization_barrier(arrays)


def delayed(x, rows):
    return jnp.pad(x[: x.shape[0] - rows], ((rows, 0), (0, 0)))


def pooled_windows(hidden, group, positions):
    values = jnp.where(positions >= 0, hidden, 0).astype(jnp.float32)
    running = values
    window_sums = jnp.zeros_like(values)
    for octave in range(GROUPS):
        running = running + delayed(running, 2**octave)
        window_sums = jnp.where(group == octave, running, window_sums)
    width = jnp.left_shift(2, group)
    counts = jnp.clip(positions + 1, 1, width).astype(jnp.float32)
    return (window_sums / counts - values).astype(jnp.bfloat16)


def per_device(stream, in_weight, out_weight, group_mix, pool_gain, norm_gain, norm_shift):
    tok_rows, width = stream.shape
    tok_half = tok_rows // 2
    at_sp = lax.axis_index("sp")
    at_tp = lax.axis_index("tp")
    core = at_tp % 2
    group = at_tp // 2
    odd = at_sp % 2
    flip = odd == 1
    alpha = (2.0 * LAYERS) ** 0.25

    weights = jnp.stack([in_weight[0], out_weight[0], in_weight[1], out_weight[1]])
    split = width // 2
    keep = jnp.where(flip, weights[..., split:], weights[..., :split])
    give = jnp.where(flip, weights[..., :split], weights[..., split:])
    traded = swapped(give, "sp")

    rows = tok_half + HALO
    sp_size, tp_size = lax.axis_size("sp"), lax.axis_size("tp")
    last = stream[tok_rows - HALO :]
    onward = [(i, i + 1) for i in range(sp_size - 1)]
    across = [
        (i * tp_size + j, (i + 1) * tp_size + (j ^ 1))
        for i in range(sp_size - 1)
        for j in range(tp_size)
    ]
    own_earlier = lax.ppermute(last, "sp", onward)
    partner_earlier = lax.ppermute(last, ("sp", "tp"), across)
    first_rows, last_rows = stream[:rows], stream[tok_rows - rows :]
    lower = core == 0
    exchanged = swapped(jnp.where(lower, last_rows, first_rows), "tp")
    traded, own_earlier, partner_earlier, exchanged = together(
        traded, own_earlier, partner_earlier, exchanged
    )
    mine = jnp.where(
        lower, jnp.concatenate([own_earlier, first_rows[:tok_half]], axis=0), last_rows
    )
    partners = jnp.where(
        lower, jnp.concatenate([partner_earlier, exchanged[:tok_half]], axis=0), exchanged
    )
    current = jnp.concatenate(
        [halves_swapped(mine, flip), halves_swapped(partners, flip)], axis=1
    )

    pair = ordered(keep, traded, flip, 1)
    first_in = lax.all_gather(
        pair[0], "sp", axis=0, axis_index_groups=every_other(), tiled=True
    )
    later = lax.all_gather(
        pair[1:], "sp", axis=1, axis_index_groups=every_other(), tiled=True
    )
    norms = jnp.stack([norm_gain, norm_shift])
    chip_count = tp_size // 2
    for layer_index in range(LAYERS):
        if layer_index == 0:
            in_quarters = all_channels(first_in)
        skipped = 0 if layer_index == 0 else HALO // 2
        sent = HALO // 2
        positions = (
            at_sp * tok_rows
            + core * tok_half
            - HALO
            + skipped
            + jnp.arange(current.shape[0], dtype=jnp.int32)
        )[:, None]
        whole_in = jnp.concatenate(in_quarters, axis=1).reshape(GROUPS, GROUP_WIDTH, 2 * width)
        partial = jnp.einsum(
            "tc,goc->gto", current, whole_in, preferred_element_type=jnp.float32
        ).astype(jnp.bfloat16)
        if layer_index == 0:
            partner_norms = swapped(after(norms, partial), "tp")
            all_norms = jnp.concatenate(
                [halves_swapped(norms, flip), halves_swapped(partner_norms, flip)], axis=-1
            )
        else:
            out_quarters = all_channels(after(later[2], partial))
        hidden = (
            between_chips(partial).astype(jnp.float32).sum(axis=0).astype(jnp.bfloat16)
        )
        pooled = pooled_windows(hidden, group, positions)[sent:]
        mixed = jnp.dot(
            pooled,
            lax.dynamic_index_in_dim(group_mix[layer_index], group, 0, keepdims=False),
            preferred_element_type=jnp.float32,
        )
        gains = lax.dynamic_slice_in_dim(
            pool_gain[layer_index], group * GROUP_WIDTH, GROUP_WIDTH
        )
        scaled = (mixed * gains[None, :]).astype(jnp.bfloat16)
        if layer_index == 0:
            everyone = between_chips(jnp.broadcast_to(scaled, (chip_count, *scaled.shape)))
            out_quarters = all_channels(later[0])
            in_quarters = all_channels(after(later[1], (everyone, out_quarters[3])))
        else:
            everyone = lax.all_gather(
                scaled[None], "tp", axis=0, axis_index_groups=chips(), tiled=True
            )
        current = current[sent:]
        whole_out = jnp.concatenate(out_quarters, axis=1).reshape(
            GROUPS, GROUP_WIDTH, 2 * width
        )
        branch = jnp.einsum(
            "gti,gic->tc", everyone, whole_out, preferred_element_type=jnp.float32
        )
        summed = alpha * current.astype(jnp.float32) + branch
        stats = jnp.stack([jnp.sum(summed, axis=1), jnp.sum(summed * summed, axis=1)])
        totals = between_chips(jnp.broadcast_to(stats, (chip_count, *stats.shape))).sum(axis=0)
        row_mean = totals[0] / D
        row_var = totals[1] / D - row_mean * row_mean
        normed = (summed - row_mean[:, None]) * lax.rsqrt(row_var + epsilon)[:, None]
        current = (
            normed * all_norms[0, layer_index][None, :] + all_norms[1, layer_index][None, :]
        ).astype(jnp.bfloat16)

    done = current
    own = halves_swapped(done[:, :width], flip)
    sent = halves_swapped(done[:, width:], flip)
    arrived = swapped(sent, "tp")
    return ordered(own, arrived, core == 1, 0)


def solution(mesh):
    in_specs = (
        P(("grp", "sp"), "tp"),
        P(None, "sp", "tp"),
        P(None, "sp", "tp"),
        P(),
        P(),
        P(None, "tp"),
        P(None, "tp"),
    )
    out_specs = P(("grp", "sp"), "tp")
    return jax.shard_map(
        per_device, mesh=mesh, in_specs=in_specs, out_specs=out_specs, check_vma=False
    )
```

```python
import jax
import jax.numpy as jnp
from jax import lax
from jax.sharding import PartitionSpec as P

D = 4096
POOL = 1024
GROUPS = 4
GROUP_WIDTH = 256
LAYERS = 2
HALO = 32

epsilon = 1e-05


def shifted(x, axis, distance):
    n = lax.axis_size(axis)
    return lax.ppermute(x, axis, [(i, (i + distance) % n) for i in range(n)])


def swapped(x, axis):
    n = lax.axis_size(axis)
    return lax.ppermute(x, axis, [(i, i ^ 1) for i in range(n)])


def chips():
    n = lax.axis_size("tp")
    return [[core + 2 * i for i in range(n // 2)] for core in range(2)]


def every_other():
    n = lax.axis_size("sp")
    return [[first + 2 * i for i in range(n // 2)] for first in range(2)]


def between_chips(x):
    return lax.all_to_all(
        x, "tp", split_axis=0, concat_axis=0, axis_index_groups=chips(), tiled=True
    )


def ordered(first, second, flip, axis):
    return jnp.where(
        flip,
        jnp.concatenate([second, first], axis=axis),
        jnp.concatenate([first, second], axis=axis),
    )


def after(x, earlier):
    return lax.optimization_barrier((x, earlier))[0]


def together(*arrays):
    return lax.optimization_barrier(arrays)


def delayed(x, rows):
    return jnp.pad(x[: x.shape[0] - rows], ((rows, 0), (0, 0)))


def pooled_windows(hidden, group, positions):
    values = jnp.where(positions >= 0, hidden, 0).astype(jnp.float32)
    running = values
    window_sums = jnp.zeros_like(values)
    for octave in range(GROUPS):
        running = running + delayed(running, 2**octave)
        window_sums = jnp.where(group == octave, running, window_sums)
    width = jnp.left_shift(2, group)
    counts = jnp.clip(positions + 1, 1, width).astype(jnp.float32)
    return (window_sums / counts - values).astype(jnp.bfloat16)


def chosen(flag, x, y):
    return jnp.where(flag, x, y)


def chip_partial(kept, sent, whole_in):
    def product(rows):
        return jnp.einsum(
            "tc,goc->gto", rows, whole_in, preferred_element_type=jnp.float32
        ).astype(jnp.bfloat16)

    arrived = swapped(product(sent), "tp")
    mine = lax.optimization_barrier(product(kept))
    return (mine.astype(jnp.float32) + arrived.astype(jnp.float32)).astype(jnp.bfloat16)


def per_device(stream, in_weight, out_weight, group_mix, pool_gain, norm_gain, norm_shift):
    tok_rows, width = stream.shape
    tok_half = tok_rows // 2
    at_sp = lax.axis_index("sp")
    at_tp = lax.axis_index("tp")
    core = at_tp % 2
    lower = core == 0
    group = at_tp // 2
    flip = at_sp % 2 == 1
    alpha = (2.0 * LAYERS) ** 0.25
    half = width // 2
    shard = in_weight.shape[1]

    def own_half(x):
        return chosen(flip, x[:, half:], x[:, :half])

    def other_half(x):
        return chosen(flip, x[:, :half], x[:, half:])

    keep = jnp.stack(
        [
            in_weight[0],
            out_weight[0],
            jnp.concatenate([own_half(in_weight[1]), own_half(out_weight[1])], axis=1),
        ]
    )
    give = jnp.stack(
        [
            in_weight[0],
            out_weight[0],
            jnp.concatenate([other_half(in_weight[1]), other_half(out_weight[1])], axis=1),
        ]
    )
    traded = swapped(give, "sp")
    last = stream[tok_rows - HALO :]
    onward = [(i, i + 1) for i in range(lax.axis_size("sp") - 1)]
    earlier = lax.ppermute(last, "sp", onward)
    traded, earlier = together(traded, earlier)

    pair = ordered(keep, traded, flip, 1)
    left_out = shard // 4
    some = chosen(flip, pair[0, left_out:], pair[0, :-left_out])
    some = lax.all_gather(
        some[None], "sp", axis=0, axis_index_groups=every_other(), tiled=True
    )
    later = lax.all_gather(
        pair[1:], "sp", axis=1, axis_index_groups=every_other(), tiled=True
    )
    lacking = swapped(chosen(flip, some[:, -left_out:], some[:, :left_out]), "sp")
    whole_in = chosen(
        flip,
        jnp.concatenate([lacking, some], axis=1),
        jnp.concatenate([some, lacking], axis=1),
    ).reshape(GROUPS, GROUP_WIDTH, width)
    whole_out = later[0].reshape(GROUPS, GROUP_WIDTH, width)

    extended = jnp.concatenate([earlier, stream], axis=0)
    rows = tok_half + HALO
    kept = chosen(lower, extended[:rows], extended[tok_half:])
    sent = chosen(lower, extended[tok_half:], extended[:rows])
    drop = HALO // 2
    for layer_index in range(LAYERS):
        positions = (
            at_sp * tok_rows
            + core * tok_half
            - HALO
            + layer_index * drop
            + jnp.arange(kept.shape[0], dtype=jnp.int32)
        )[:, None]
        partial = chip_partial(kept, sent, whole_in)
        hidden = (
            between_chips(partial).astype(jnp.float32).sum(axis=0).astype(jnp.bfloat16)
        )
        pooled = pooled_windows(hidden, group, positions)[drop:]
        mixed = jnp.dot(
            pooled,
            lax.dynamic_index_in_dim(group_mix[layer_index], group, 0, keepdims=False),
            preferred_element_type=jnp.float32,
        )
        gains = lax.dynamic_slice_in_dim(
            pool_gain[layer_index], group * GROUP_WIDTH, GROUP_WIDTH
        )
        scaled = (mixed * gains[None, :]).astype(jnp.bfloat16)
        own_rows = lax.all_gather(
            scaled[None], "tp", axis=0, axis_index_groups=chips(), tiled=True
        )
        other_rows = swapped(own_rows, "tp")
        if layer_index == 1:
            whole_out = ordered(later[1][:, half:], others[:, half:], flip, 1)
            whole_out = whole_out.reshape(GROUPS, GROUP_WIDTH, width)

        def layer_sum(everyone, current):
            branch = jnp.einsum(
                "gti,gic->tc", everyone, whole_out, preferred_element_type=jnp.float32
            )
            summed = alpha * current.astype(jnp.float32) + branch
            return summed, jnp.stack(
                [jnp.sum(summed, axis=1), jnp.sum(summed * summed, axis=1)]
            )

        own_sum, own_stats = layer_sum(own_rows, kept[drop:])
        other_sum, other_stats = layer_sum(other_rows, sent[drop:])
        stats = jnp.stack([chosen(lower, own_stats, other_stats), chosen(lower, other_stats, own_stats)])
        count = lax.axis_size("tp")
        totals = lax.all_to_all(
            jnp.broadcast_to(stats, (count, *stats.shape)),
            "tp",
            split_axis=0,
            concat_axis=0,
            tiled=True,
        ).sum(axis=0)
        own_totals = chosen(lower, totals[0], totals[1])
        other_totals = chosen(lower, totals[1], totals[0])
        if layer_index == 0:
            source = after(later[1], other_stats)
            middle = source.shape[0] // 2
            low = shifted(source[:middle], "sp", 1)
            high = shifted(source[middle:], "sp", -1)
            others = jnp.concatenate([low, high], axis=0)
            whole_in = ordered(source[:, :half], others[:, :half], flip, 1)
            whole_in = whole_in.reshape(GROUPS, GROUP_WIDTH, width)

        def normalised(summed, sums):
            row_mean = sums[0] / D
            row_var = sums[1] / D - row_mean * row_mean
            normed = (summed - row_mean[:, None]) * lax.rsqrt(row_var + epsilon)[:, None]
            return (
                normed * norm_gain[layer_index][None, :] + norm_shift[layer_index][None, :]
            ).astype(jnp.bfloat16)

        kept = normalised(own_sum, own_totals)
        sent = normalised(other_sum, other_totals)

    return ordered(kept, sent, core == 1, 0)


def solution(mesh):
    in_specs = (
        P(("grp", "sp"), "tp"),
        P(None, "sp", "tp"),
        P(None, "sp", "tp"),
        P(),
        P(),
        P(None, "tp"),
        P(None, "tp"),
    )
    out_specs = P(("grp", "sp"), "tp")
    return jax.shard_map(
        per_device, mesh=mesh, in_specs=in_specs, out_specs=out_specs, check_vma=False
    )
```

```python
import jax
import jax.numpy as jnp
from jax import lax
from jax.sharding import PartitionSpec as P

D = 4096
POOL = 1024
GROUPS = 4
GROUP_WIDTH = 256
LAYERS = 2
HALO = 32

epsilon = 1e-05


def shifted(x, axis, distance):
    n = lax.axis_size(axis)
    return lax.ppermute(x, axis, [(i, (i + distance) % n) for i in range(n)])


def swapped(x, axis):
    n = lax.axis_size(axis)
    return lax.ppermute(x, axis, [(i, i ^ 1) for i in range(n)])


def chips():
    n = lax.axis_size("tp")
    return [[core + 2 * i for i in range(n // 2)] for core in range(2)]


def every_other():
    n = lax.axis_size("sp")
    return [[first + 2 * i for i in range(n // 2)] for first in range(2)]


def between_chips(x):
    return lax.all_to_all(
        x, "tp", split_axis=0, concat_axis=0, axis_index_groups=chips(), tiled=True
    )


def ordered(first, second, flip, axis):
    return jnp.where(
        flip,
        jnp.concatenate([second, first], axis=axis),
        jnp.concatenate([first, second], axis=axis),
    )


def after(x, earlier):
    return lax.optimization_barrier((x, earlier))[0]


def together(*arrays):
    return lax.optimization_barrier(arrays)


def delayed(x, rows):
    return jnp.pad(x[: x.shape[0] - rows], ((rows, 0), (0, 0)))


def pooled_windows(hidden, group, positions):
    values = jnp.where(positions >= 0, hidden, 0).astype(jnp.float32)
    running = values
    window_sums = jnp.zeros_like(values)
    for octave in range(GROUPS):
        running = running + delayed(running, 2**octave)
        window_sums = jnp.where(group == octave, running, window_sums)
    width = jnp.left_shift(2, group)
    counts = jnp.clip(positions + 1, 1, width).astype(jnp.float32)
    return (window_sums / counts - values).astype(jnp.bfloat16)


def chosen(flag, x, y):
    return jnp.where(flag, x, y)


def chip_partial(kept, sent, whole_in):
    def product(rows):
        return jnp.einsum(
            "tc,goc->gto", rows, whole_in, preferred_element_type=jnp.float32
        ).astype(jnp.bfloat16)

    arrived = swapped(product(sent), "tp")
    mine = lax.optimization_barrier(product(kept))
    return (mine.astype(jnp.float32) + arrived.astype(jnp.float32)).astype(jnp.bfloat16)


def per_device(stream, in_weight, out_weight, group_mix, pool_gain, norm_gain, norm_shift):
    tok_rows, width = stream.shape
    tok_half = tok_rows // 2
    at_sp = lax.axis_index("sp")
    at_tp = lax.axis_index("tp")
    core = at_tp % 2
    lower = core == 0
    group = at_tp // 2
    flip = at_sp % 2 == 1
    alpha = (2.0 * LAYERS) ** 0.25
    shard = in_weight.shape[1]

    first_in = lax.all_gather(
        in_weight[0], "sp", axis=0, axis_index_groups=every_other(), tiled=True
    )
    later = lax.all_gather(
        jnp.concatenate([out_weight[0], in_weight[1], out_weight[1]], axis=1),
        "sp",
        axis=0,
        axis_index_groups=every_other(),
        tiled=True,
    )

    def from_neighbours(own, *more):
        middle = own.shape[0] // 2
        low = shifted(jnp.concatenate([own[:middle], *more], axis=0), "sp", 1)
        high = shifted(own[middle:], "sp", -1)
        others = jnp.concatenate([low[:middle], high], axis=0)
        columns = own.shape[1]
        whole = ordered(
            own.reshape(-1, shard, columns), others.reshape(-1, shard, columns), flip, 1
        )
        return whole.reshape(GROUPS, GROUP_WIDTH, columns), low[middle:]

    whole_in, earlier = from_neighbours(first_in, stream[tok_rows - HALO :])
    extended = jnp.concatenate([earlier, stream], axis=0)
    rows = tok_half + HALO
    kept = chosen(lower, extended[:rows], extended[tok_half:])
    sent = chosen(lower, extended[tok_half:], extended[:rows])
    drop = HALO // 2
    for layer_index in range(LAYERS):
        positions = (
            at_sp * tok_rows
            + core * tok_half
            - HALO
            + layer_index * drop
            + jnp.arange(kept.shape[0], dtype=jnp.int32)
        )[:, None]
        partial = chip_partial(kept, sent, whole_in)
        pieces = between_chips(partial)
        if layer_index == 1:
            whole_out, _ = from_neighbours(after(later[:, 2 * width :], partial))
            pieces, whole_out = together(pieces, whole_out)
        hidden = pieces.astype(jnp.float32).sum(axis=0).astype(jnp.bfloat16)
        pooled = pooled_windows(hidden, group, positions)[drop:]
        mixed = jnp.dot(
            pooled,
            lax.dynamic_index_in_dim(group_mix[layer_index], group, 0, keepdims=False),
            preferred_element_type=jnp.float32,
        )
        gains = lax.dynamic_slice_in_dim(
            pool_gain[layer_index], group * GROUP_WIDTH, GROUP_WIDTH
        )
        scaled = (mixed * gains[None, :]).astype(jnp.bfloat16)
        if layer_index == 0:
            own_rows = between_chips(
                jnp.broadcast_to(scaled, (lax.axis_size("tp") // 2, *scaled.shape))
            )
            ready = after(later[:, : 2 * width], scaled)
            both, _ = from_neighbours(ready)
            whole_out, next_in = both[..., :width], both[..., width:]
        else:
            own_rows = lax.all_gather(
                scaled[None], "tp", axis=0, axis_index_groups=chips(), tiled=True
            )
        other_rows = swapped(own_rows, "tp")
        def layer_sum(everyone, current):
            branch = jnp.einsum(
                "gti,gic->tc", everyone, whole_out, preferred_element_type=jnp.float32
            )
            summed = alpha * current.astype(jnp.float32) + branch
            return summed, jnp.stack(
                [jnp.sum(summed, axis=1), jnp.sum(summed * summed, axis=1)]
            )

        own_sum, own_stats = layer_sum(own_rows, kept[drop:])
        other_sum, other_stats = layer_sum(other_rows, sent[drop:])
        stats = jnp.stack([chosen(lower, own_stats, other_stats), chosen(lower, other_stats, own_stats)])
        count = lax.axis_size("tp")
        totals = lax.all_to_all(
            jnp.broadcast_to(stats, (count, *stats.shape)),
            "tp",
            split_axis=0,
            concat_axis=0,
            tiled=True,
        ).sum(axis=0)
        own_totals = chosen(lower, totals[0], totals[1])
        other_totals = chosen(lower, totals[1], totals[0])
        def normalised(summed, sums):
            row_mean = sums[0] / D
            row_var = sums[1] / D - row_mean * row_mean
            normed = (summed - row_mean[:, None]) * lax.rsqrt(row_var + epsilon)[:, None]
            return (
                normed * norm_gain[layer_index][None, :] + norm_shift[layer_index][None, :]
            ).astype(jnp.bfloat16)

        kept = normalised(own_sum, own_totals)
        sent = normalised(other_sum, other_totals)
        whole_in = next_in

    return ordered(kept, sent, core == 1, 0)


def solution(mesh):
    in_specs = (
        P(("grp", "sp"), "tp"),
        P(None, "sp", "tp"),
        P(None, "sp", "tp"),
        P(),
        P(),
        P(None, "tp"),
        P(None, "tp"),
    )
    out_specs = P(("grp", "sp"), "tp")
    return jax.shard_map(
        per_device, mesh=mesh, in_specs=in_specs, out_specs=out_specs, check_vma=False
    )
```

```python
import jax
import jax.numpy as jnp
from jax import lax
from jax.sharding import PartitionSpec as P

D = 4096
GROUPS = 4
GROUP_WIDTH = 256
LAYERS = 2
HALO = 32

epsilon = 1e-05


def shifted(x, axis, distance):
    n = lax.axis_size(axis)
    return lax.ppermute(x, axis, [(i, (i + distance) % n) for i in range(n)])


def swapped(x, axis):
    n = lax.axis_size(axis)
    return lax.ppermute(x, axis, [(i, i ^ 1) for i in range(n)])


def chips():
    n = lax.axis_size("tp")
    return [[core + 2 * i for i in range(n // 2)] for core in range(2)]


def every_other():
    n = lax.axis_size("sp")
    return [[first + 2 * i for i in range(n // 2)] for first in range(2)]


def between_chips(x):
    return lax.all_to_all(
        x, "tp", split_axis=0, concat_axis=0, axis_index_groups=chips(), tiled=True
    )


def ordered(first, second, flip, axis):
    return jnp.where(
        flip,
        jnp.concatenate([second, first], axis=axis),
        jnp.concatenate([first, second], axis=axis),
    )


def delayed(x, rows):
    return jnp.pad(x[: x.shape[0] - rows], ((rows, 0), (0, 0)))


def pooled_windows(hidden, group, positions):
    values = jnp.where(positions >= 0, hidden, 0).astype(jnp.float32)
    running = values
    window_sums = jnp.zeros_like(values)
    for octave in range(GROUPS):
        running = running + delayed(running, 2**octave)
        window_sums = jnp.where(group == octave, running, window_sums)
    width = jnp.left_shift(2, group)
    counts = jnp.clip(positions + 1, 1, width).astype(jnp.float32)
    return (window_sums / counts - values).astype(jnp.bfloat16)


def chosen(flag, x, y):
    return jnp.where(flag, x, y)


def chip_partial(kept, sent, whole_in):
    def product(rows):
        return jnp.einsum("tc,goc->gto", rows, whole_in, preferred_element_type=jnp.float32)

    arrived = swapped(product(sent).astype(jnp.bfloat16), "tp")
    return (product(kept) + arrived.astype(jnp.float32)).astype(jnp.bfloat16)


def per_device(stream, in_weight, out_weight, group_mix, pool_gain, norm_gain, norm_shift):
    tok_rows, width = stream.shape
    tok_half = tok_rows // 2
    at_sp = lax.axis_index("sp")
    at_tp = lax.axis_index("tp")
    core = at_tp % 2
    lower = core == 0
    group = at_tp // 2
    flip = at_sp % 2 == 1
    alpha = (2.0 * LAYERS) ** 0.25
    shard = in_weight.shape[1]

    first_in = lax.all_gather(
        in_weight[0], "sp", axis=0, axis_index_groups=every_other(), tiled=True
    )
    later = lax.all_gather(
        jnp.concatenate([out_weight[0], in_weight[1], out_weight[1]], axis=1),
        "sp",
        axis=0,
        axis_index_groups=every_other(),
        tiled=True,
    )

    def interleaved(own, others):
        whole = ordered(own.reshape(-1, shard, width), others.reshape(-1, shard, width), flip, 1)
        return whole.reshape(GROUPS, GROUP_WIDTH, width)

    def from_neighbours(own, *more):
        middle = own.shape[0] // 2
        low = shifted(jnp.concatenate([own[:middle], *more], axis=0), "sp", 1)
        high = shifted(own[middle:], "sp", -1)
        others = jnp.concatenate([low[:middle], high], axis=0)
        return interleaved(own, others), low[middle:]

    def from_partner(own):
        return interleaved(own, swapped(own, "sp"))

    whole_in, earlier = from_neighbours(first_in, stream[tok_rows - HALO :])
    extended = jnp.concatenate([earlier, stream], axis=0)
    rows = tok_half + HALO
    kept = chosen(lower, extended[:rows], extended[tok_half:])
    sent = chosen(lower, extended[tok_half:], extended[:rows])
    drop = HALO // 2
    for layer_index in range(LAYERS):
        positions = (
            at_sp * tok_rows
            + core * tok_half
            - HALO
            + layer_index * drop
            + jnp.arange(kept.shape[0], dtype=jnp.int32)
        )[:, None]
        partial = chip_partial(kept, sent, whole_in)
        pieces = between_chips(partial)
        if layer_index == 1:
            whole_out = from_partner(later[:, 2 * width :])
        hidden = pieces.astype(jnp.float32).sum(axis=0).astype(jnp.bfloat16)
        pooled = pooled_windows(hidden, group, positions)[drop:]
        mixed = jnp.dot(
            pooled,
            lax.dynamic_index_in_dim(group_mix[layer_index], group, 0, keepdims=False),
            preferred_element_type=jnp.float32,
        )
        gains = lax.dynamic_slice_in_dim(
            pool_gain[layer_index], group * GROUP_WIDTH, GROUP_WIDTH
        )
        scaled = (mixed * gains[None, :]).astype(jnp.bfloat16)
        if layer_index == 0:
            copies = jnp.broadcast_to(scaled, (lax.axis_size("tp") // 2, *scaled.shape))
            own_rows = between_chips(copies)
            whole_out, _ = from_neighbours(later[:, :width])
        else:
            own_rows = lax.all_gather(
                scaled[None], "tp", axis=0, axis_index_groups=chips(), tiled=True
            )
        other_rows = swapped(own_rows, "tp")

        def layer_sum(everyone, current):
            branch = jnp.einsum(
                "gti,gic->tc", everyone, whole_out, preferred_element_type=jnp.float32
            )
            summed = alpha * current.astype(jnp.float32) + branch
            return summed, jnp.stack(
                [jnp.sum(summed, axis=1), jnp.sum(summed * summed, axis=1)]
            )

        own_sum, own_stats = layer_sum(own_rows, kept[drop:])
        other_sum, other_stats = layer_sum(other_rows, sent[drop:])
        if layer_index == 0:
            next_in = from_partner(later[:, width : 2 * width])
        stats = jnp.stack([chosen(lower, own_stats, other_stats), chosen(lower, other_stats, own_stats)])
        count = lax.axis_size("tp")
        everyones = lax.all_to_all(
            jnp.broadcast_to(stats, (count, *stats.shape)),
            "tp",
            split_axis=0,
            concat_axis=0,
            tiled=True,
        )
        totals = everyones.sum(axis=0)
        own_totals = chosen(lower, totals[0], totals[1])
        other_totals = chosen(lower, totals[1], totals[0])

        def normalised(summed, sums):
            row_mean = sums[0] / D
            row_var = sums[1] / D - row_mean * row_mean
            normed = (summed - row_mean[:, None]) * lax.rsqrt(row_var + epsilon)[:, None]
            return (
                normed * norm_gain[layer_index][None, :] + norm_shift[layer_index][None, :]
            ).astype(jnp.bfloat16)

        kept = normalised(own_sum, own_totals)
        sent = normalised(other_sum, other_totals)
        whole_in = next_in

    return ordered(kept, sent, core == 1, 0)


def solution(mesh):
    in_specs = (
        P(("grp", "sp"), "tp"),
        P(None, "sp", "tp"),
        P(None, "sp", "tp"),
        P(),
        P(),
        P(None, "tp"),
        P(None, "tp"),
    )
    out_specs = P(("grp", "sp"), "tp")

    return jax.shard_map(
        per_device, mesh=mesh, in_specs=in_specs, out_specs=out_specs, check_vma=False
    )
```

```python
import jax
import jax.numpy as jnp
from jax import lax
from jax.sharding import PartitionSpec as P

D = 4096
GROUPS = 4
GROUP_WIDTH = 256
LAYERS = 2
HALO = 32

epsilon = 1e-05


def shifted(x, axis, distance):
    n = lax.axis_size(axis)
    return lax.ppermute(x, axis, [(i, (i + distance) % n) for i in range(n)])


def swapped(x, axis):
    n = lax.axis_size(axis)
    return lax.ppermute(x, axis, [(i, i ^ 1) for i in range(n)])


def chips():
    n = lax.axis_size("tp")
    return [[core + 2 * i for i in range(n // 2)] for core in range(2)]


def every_other():
    n = lax.axis_size("sp")
    return [[first + 2 * i for i in range(n // 2)] for first in range(2)]


def between_chips(x):
    return lax.all_to_all(
        x, "tp", split_axis=0, concat_axis=0, axis_index_groups=chips(), tiled=True
    )


def ordered(first, second, flip, axis):
    return jnp.where(
        flip,
        jnp.concatenate([second, first], axis=axis),
        jnp.concatenate([first, second], axis=axis),
    )


def delayed(x, rows):
    return jnp.pad(x[: x.shape[0] - rows], ((rows, 0), (0, 0)))


def pooled_windows(hidden, group, positions):
    values = jnp.where(positions >= 0, hidden, 0).astype(jnp.float32)
    running = values
    window_sums = jnp.zeros_like(values)
    for octave in range(GROUPS):
        running = running + delayed(running, 2**octave)
        window_sums = jnp.where(group == octave, running, window_sums)
    width = jnp.left_shift(2, group)
    counts = jnp.clip(positions + 1, 1, width).astype(jnp.float32)
    return (window_sums / counts - values).astype(jnp.bfloat16)


def chosen(flag, x, y):
    return jnp.where(flag, x, y)


def chip_partial(kept, sent, whole_in):
    def product(rows):
        return jnp.einsum("tc,goc->gto", rows, whole_in, preferred_element_type=jnp.float32)

    arrived = swapped(product(sent).astype(jnp.bfloat16), "tp")
    return (product(kept) + arrived.astype(jnp.float32)).astype(jnp.bfloat16)


def per_device(stream, in_weight, out_weight, group_mix, pool_gain, norm_gain, norm_shift):
    tok_rows, width = stream.shape
    tok_half = tok_rows // 2
    at_sp = lax.axis_index("sp")
    at_tp = lax.axis_index("tp")
    core = at_tp % 2
    lower = core == 0
    group = at_tp // 2
    flip = at_sp % 2 == 1
    alpha = (2.0 * LAYERS) ** 0.25
    shard = in_weight.shape[1]

    first_in = lax.all_gather(
        in_weight[0], "sp", axis=0, axis_index_groups=every_other(), tiled=True
    )
    later = lax.all_gather(
        jnp.concatenate([out_weight, in_weight[1:]], axis=0),
        "sp",
        axis=1,
        axis_index_groups=every_other(),
        tiled=True,
    )

    def interleaved(own, others):
        whole = ordered(own.reshape(-1, shard, width), others.reshape(-1, shard, width), flip, 1)
        return whole.reshape(GROUPS, GROUP_WIDTH, width)

    def from_neighbours(own, *more):
        middle = own.shape[0] // 2
        low = shifted(jnp.concatenate([own[:middle], *more], axis=0), "sp", 1)
        high = shifted(own[middle:], "sp", -1)
        others = jnp.concatenate([low[:middle], high], axis=0)
        return interleaved(own, others), low[middle:]

    def from_partner(own):
        return interleaved(own, swapped(own, "sp"))

    whole_in, earlier = from_neighbours(first_in, stream[tok_rows - HALO :])
    extended = jnp.concatenate([earlier, stream], axis=0)
    rows = tok_half + HALO
    kept = chosen(lower, extended[:rows], extended[tok_half:])
    sent = chosen(lower, extended[tok_half:], extended[:rows])
    drop = HALO // 2
    for layer_index in range(LAYERS):
        positions = (
            at_sp * tok_rows
            + core * tok_half
            - HALO
            + layer_index * drop
            + jnp.arange(kept.shape[0], dtype=jnp.int32)
        )[:, None]
        partial = chip_partial(kept, sent, whole_in)
        pieces = between_chips(partial)
        if layer_index == 1:
            whole_out = from_partner(later[1])
        hidden = pieces.astype(jnp.float32).sum(axis=0).astype(jnp.bfloat16)
        pooled = pooled_windows(hidden, group, positions)[drop:]
        mixed = jnp.dot(
            pooled,
            lax.dynamic_index_in_dim(group_mix[layer_index], group, 0, keepdims=False),
            preferred_element_type=jnp.float32,
        )
        gains = lax.dynamic_slice_in_dim(
            pool_gain[layer_index], group * GROUP_WIDTH, GROUP_WIDTH
        )
        scaled = (mixed * gains[None, :]).astype(jnp.bfloat16)
        if layer_index == 0:
            copies = jnp.broadcast_to(scaled, (lax.axis_size("tp") // 2, *scaled.shape))
            own_rows = between_chips(copies)
            whole_out, _ = from_neighbours(later[0])
        else:
            own_rows = lax.all_gather(
                scaled[None], "tp", axis=0, axis_index_groups=chips(), tiled=True
            )
        other_rows = swapped(own_rows, "tp")

        def layer_sum(everyone, current):
            branch = jnp.einsum(
                "gti,gic->tc", everyone, whole_out, preferred_element_type=jnp.float32
            )
            summed = alpha * current.astype(jnp.float32) + branch
            return summed, jnp.stack(
                [jnp.sum(summed, axis=1), jnp.sum(summed * summed, axis=1)]
            )

        own_sum, own_stats = layer_sum(own_rows, kept[drop:])
        other_sum, other_stats = layer_sum(other_rows, sent[drop:])
        if layer_index == 0:
            next_in = from_partner(later[2])
        stats = jnp.stack([chosen(lower, own_stats, other_stats), chosen(lower, other_stats, own_stats)])
        count = lax.axis_size("tp")
        everyones = lax.all_to_all(
            jnp.broadcast_to(stats, (count, *stats.shape)),
            "tp",
            split_axis=0,
            concat_axis=0,
            tiled=True,
        )
        totals = everyones.sum(axis=0)
        own_totals = chosen(lower, totals[0], totals[1])
        other_totals = chosen(lower, totals[1], totals[0])

        def normalised(summed, sums):
            row_mean = sums[0] / D
            row_var = sums[1] / D - row_mean * row_mean
            normed = (summed - row_mean[:, None]) * lax.rsqrt(row_var + epsilon)[:, None]
            return (
                normed * norm_gain[layer_index][None, :] + norm_shift[layer_index][None, :]
            ).astype(jnp.bfloat16)

        if layer_index == LAYERS - 1:
            sums = ordered(own_sum, other_sum, core == 1, 0)
            return normalised(sums, jnp.concatenate([totals[0], totals[1]], axis=1))
        kept = normalised(own_sum, own_totals)
        sent = normalised(other_sum, other_totals)
        whole_in = next_in


def solution(mesh):
    in_specs = (
        P(("grp", "sp"), "tp"),
        P(None, "sp", "tp"),
        P(None, "sp", "tp"),
        P(),
        P(),
        P(None, "tp"),
        P(None, "tp"),
    )
    out_specs = P(("grp", "sp"), "tp")

    return jax.shard_map(
        per_device, mesh=mesh, in_specs=in_specs, out_specs=out_specs, check_vma=False
    )
```

```python
import jax
import jax.numpy as jnp
from jax import lax
from jax.sharding import PartitionSpec as P

D = 4096
GROUPS = 4
GROUP_WIDTH = 256
LAYERS = 2
HALO = 32

epsilon = 1e-05


def shifted(x, axis, distance):
    n = lax.axis_size(axis)
    return lax.ppermute(x, axis, [(i, (i + distance) % n) for i in range(n)])


def swapped(x, axis):
    n = lax.axis_size(axis)
    return lax.ppermute(x, axis, [(i, i ^ 1) for i in range(n)])


def chips():
    n = lax.axis_size("tp")
    return [[core + 2 * i for i in range(n // 2)] for core in range(2)]


def every_other():
    n = lax.axis_size("sp")
    return [[first + 2 * i for i in range(n // 2)] for first in range(2)]


def between_chips(x):
    return lax.all_to_all(
        x, "tp", split_axis=0, concat_axis=0, axis_index_groups=chips(), tiled=True
    )


def ordered(first, second, flip, axis):
    return jnp.where(
        flip,
        jnp.concatenate([second, first], axis=axis),
        jnp.concatenate([first, second], axis=axis),
    )


def delayed(x, rows):
    return jnp.pad(x[: x.shape[0] - rows], ((rows, 0), (0, 0)))


def pooled_windows(hidden, group, positions):
    values = jnp.where(positions >= 0, hidden, 0).astype(jnp.float32)
    running = values
    window_sums = jnp.zeros_like(values)
    for octave in range(GROUPS):
        running = running + delayed(running, 2**octave)
        window_sums = jnp.where(group == octave, running, window_sums)
    width = jnp.left_shift(2, group)
    counts = jnp.clip(positions + 1, 1, width).astype(jnp.float32)
    return (window_sums / counts - values).astype(jnp.bfloat16)


def chosen(flag, x, y):
    return jnp.where(flag, x, y)


def chip_partial(kept, sent, whole_in):
    def product(rows):
        return jnp.einsum("tc,goc->gto", rows, whole_in, preferred_element_type=jnp.float32)

    arrived = swapped(product(sent).astype(jnp.bfloat16), "tp")
    return (product(kept) + arrived.astype(jnp.float32)).astype(jnp.bfloat16)


def per_device(stream, in_weight, out_weight, group_mix, pool_gain, norm_gain, norm_shift):
    tok_rows, width = stream.shape
    tok_half = tok_rows // 2
    at_sp = lax.axis_index("sp")
    at_tp = lax.axis_index("tp")
    core = at_tp % 2
    lower = core == 0
    group = at_tp // 2
    flip = at_sp % 2 == 1
    alpha = (2.0 * LAYERS) ** 0.25
    shard = in_weight.shape[1]

    first_in = lax.all_gather(
        in_weight[0], "sp", axis=0, axis_index_groups=every_other(), tiled=True
    )
    upper = lax.axis_index("grp") % 2 == 1
    half = width // 2
    last_half = chosen(upper, out_weight[1][:, half:], out_weight[1][:, :half])
    later = lax.all_gather(
        jnp.concatenate([out_weight[0], in_weight[1], last_half], axis=1),
        "sp",
        axis=0,
        axis_index_groups=every_other(),
        tiled=True,
    )

    def interleaved(own, others):
        whole = ordered(own.reshape(-1, shard, width), others.reshape(-1, shard, width), flip, 1)
        return whole.reshape(GROUPS, GROUP_WIDTH, width)

    def from_neighbours(own, *more):
        middle = own.shape[0] // 2
        low = shifted(jnp.concatenate([own[:middle], *more], axis=0), "sp", 1)
        high = shifted(own[middle:], "sp", -1)
        others = jnp.concatenate([low[:middle], high], axis=0)
        return interleaved(own, others), low[middle:]

    def from_partner(own):
        return interleaved(own, swapped(own, "sp"))

    whole_in, earlier = from_neighbours(first_in, stream[tok_rows - HALO :])
    extended = jnp.concatenate([earlier, stream], axis=0)
    rows = tok_half + HALO
    kept = chosen(lower, extended[:rows], extended[tok_half:])
    sent = chosen(lower, extended[tok_half:], extended[:rows])
    drop = HALO // 2
    for layer_index in range(LAYERS):
        positions = (
            at_sp * tok_rows
            + core * tok_half
            - HALO
            + layer_index * drop
            + jnp.arange(kept.shape[0], dtype=jnp.int32)
        )[:, None]
        partial = chip_partial(kept, sent, whole_in)
        pieces = between_chips(partial)
        if layer_index == 1:
            own_half = later[:, 2 * width :]
            rows_here = ordered(own_half, paired_half, upper, 1)
            whole_out = from_partner(rows_here)
        hidden = pieces.astype(jnp.float32).sum(axis=0).astype(jnp.bfloat16)
        pooled = pooled_windows(hidden, group, positions)[drop:]
        mixed = jnp.dot(
            pooled,
            lax.dynamic_index_in_dim(group_mix[layer_index], group, 0, keepdims=False),
            preferred_element_type=jnp.float32,
        )
        gains = lax.dynamic_slice_in_dim(
            pool_gain[layer_index], group * GROUP_WIDTH, GROUP_WIDTH
        )
        scaled = (mixed * gains[None, :]).astype(jnp.bfloat16)
        if layer_index == 0:
            copies = jnp.broadcast_to(scaled, (lax.axis_size("tp") // 2, *scaled.shape))
            own_rows = between_chips(copies)
            whole_out, _ = from_neighbours(later[:, :width])
        else:
            own_rows = lax.all_gather(
                scaled[None], "tp", axis=0, axis_index_groups=chips(), tiled=True
            )
        other_rows = swapped(own_rows, "tp")

        def layer_sum(everyone, current):
            branch = jnp.einsum(
                "gti,gic->tc", everyone, whole_out, preferred_element_type=jnp.float32
            )
            summed = alpha * current.astype(jnp.float32) + branch
            return summed, jnp.stack(
                [jnp.sum(summed, axis=1), jnp.sum(summed * summed, axis=1)]
            )

        own_sum, own_stats = layer_sum(own_rows, kept[drop:])
        other_sum, other_stats = layer_sum(other_rows, sent[drop:])
        if layer_index == 0:
            next_in = from_partner(later[:, width : 2 * width])
            paired_half = swapped(later[:, 2 * width :], "grp")
        stats = jnp.stack([chosen(lower, own_stats, other_stats), chosen(lower, other_stats, own_stats)])
        count = lax.axis_size("tp")
        everyones = lax.all_to_all(
            jnp.broadcast_to(stats, (count, *stats.shape)),
            "tp",
            split_axis=0,
            concat_axis=0,
            tiled=True,
        )
        totals = everyones.sum(axis=0)
        own_totals = chosen(lower, totals[0], totals[1])
        other_totals = chosen(lower, totals[1], totals[0])

        def normalised(summed, sums):
            row_mean = sums[0] / D
            row_var = sums[1] / D - row_mean * row_mean
            normed = (summed - row_mean[:, None]) * lax.rsqrt(row_var + epsilon)[:, None]
            return (
                normed * norm_gain[layer_index][None, :] + norm_shift[layer_index][None, :]
            ).astype(jnp.bfloat16)

        if layer_index == LAYERS - 1:
            sums = ordered(own_sum, other_sum, core == 1, 0)
            return normalised(sums, jnp.concatenate([totals[0], totals[1]], axis=1))
        kept = normalised(own_sum, own_totals)
        sent = normalised(other_sum, other_totals)
        whole_in = next_in


def solution(mesh):
    in_specs = (
        P(("grp", "sp"), "tp"),
        P(None, "sp", "tp"),
        P(None, "sp", "tp"),
        P(),
        P(),
        P(None, "tp"),
        P(None, "tp"),
    )
    out_specs = P(("grp", "sp"), "tp")

    return jax.shard_map(
        per_device, mesh=mesh, in_specs=in_specs, out_specs=out_specs, check_vma=False
    )
```
